32 devices in a mesh: rep: 2 (over x), fs: 8 (over z, y), tp: 2 (over core).
Axes of the slice: x: 2, y: 2, z: 4, core: 2. Of those that a mesh axis runs over, the one named last changes fastest.
Arguments:
- late_rows: bfloat16 [4096, 2048], P(('rep', 'fs')), parts along dimension 0, may hold values from -6 to 6
- early_rows: bfloat16 [4096, 2048], P(('rep', 'fs')), parts along dimension 0, may hold values from -6 to 6
- hidden_cot: bfloat16 [4096, 5632], P(('rep', 'fs'), 'tp'), parts along dimension 0, may hold values from -6 to 6
- gate_weight: bfloat16 [2048, 5632], P('fs', 'tp'), may hold values from -0.125 to 0.125
- up_weight: bfloat16 [2048, 5632], P('fs', 'tp'), may hold values from -0.125 to 0.125
- gate_taps: bfloat16 [3, 5632], P(None, 'tp'), may hold values from -3.5 to 3.5
- up_taps: bfloat16 [3, 5632], P(None, 'tp'), may hold values from -3.5 to 3.5
- gate_grad_sum: float32 [4096, 5632], P(('rep', 'fs'), 'tp'), parts along dimension 0, may hold values from -6 to 6
- up_grad_sum: float32 [4096, 5632], P(('rep', 'fs'), 'tp'), parts along dimension 0, may hold values from -6 to 6
- gate_taps_sum: float32 [6, 5632], P('rep', 'tp'), parts along dimension 0, may hold values from -6 to 6
- up_taps_sum: float32 [6, 5632], P('rep', 'tp'), parts along dimension 0, may hold values from -6 to 6
Outputs:
- late_hidden: bfloat16 [4096, 5632], P(('rep', 'fs'), 'tp'), parts along dimension 0
- early_grad: bfloat16 [4096, 2048], P(('rep', 'fs')), parts along dimension 0
- gate_grad_next: float32 [4096, 5632], P(('rep', 'fs'), 'tp'), parts along dimension 0
- up_grad_next: float32 [4096, 5632], P(('rep', 'fs'), 'tp'), parts along dimension 0
- gate_taps_next: float32 [6, 5632], P('rep', 'tp'), parts along dimension 0
- up_taps_next: float32 [6, 5632], P('rep', 'tp'), parts along dimension 0
The draws below stay inside these ranges and needn't reach their ends.
There are 2 independent parts, one for each index of `rep`. The reference program is written for one: setup_inputs(seed, part) draws one part's arguments, and reference() takes and returns one part's arrays. A program takes and returns all parts, laid end to end along the dimension named above; an argument that names none is the same for every part. Nothing has to cross between parts.
All inputs are finite; a program needn't handle non-finite values.
Results may differ from the reference program's by a relative error of at most 0.02.
Values may be sent and summed in bfloat16 or wider, within the bound.
A program may use at most 128 MiB of HBM per device.

```python
import jax
import jax.numpy as jnp
from jax import lax

D = 2048
FF = 5632
TAPS = 3
TOK_DEV = 256
TOKENS = 2048
N_FS = 8


def strengthened(entries, stream_key, source, target, shards_of, factor):
    owner, partner = [(jnp.arange(entries.shape[position]) // (entries.shape[position] // shards_of)).reshape([-1 if axis == position else 1 for axis in range(entries.ndim)]) for position in (source, target)]
    chosen = jax.random.permutation(stream_key, shards_of)[partner]
    strong = (owner == chosen) | (owner == (partner + shards_of // 2) % shards_of)
    return jnp.where(strong, factor * entries, entries)


def levels(own_key, dims, pieces, least, high):
    def one(axis_at, parts):
        steps = jax.random.uniform(jax.random.fold_in(jax.random.fold_in(own_key, 6), axis_at), (parts,), jnp.float32, least / len(pieces), high / len(pieces))
        return jnp.repeat(jnp.exp(steps), dims[axis_at] // parts).reshape((-1,) + (1,) * (len(dims) - axis_at - 1))

    level = one(*pieces[0])
    for cut in pieces[1:]:
        level = level * one(*cut)
    return level


def bell_draw(own_key, shape, spread, bound, cuts=(), dtype=jnp.bfloat16):
    gain = levels(own_key, shape, cuts, -0.22, 0.18) if cuts else 1.0
    drawn = jax.random.normal(own_key, shape, jnp.float32) * spread * gain
    return jnp.minimum(jnp.maximum(drawn, -bound), bound).astype(dtype)


def bell_draw_with(rng, extent, width, bound, pieces, heavy, held_as=jnp.bfloat16):
    drawn = width * jax.random.normal(rng, extent, jnp.float32)
    if pieces:
        drawn = drawn * levels(rng, extent, pieces, -0.22, 0.18)
    return jnp.clip(strengthened(drawn, jax.random.fold_in(rng, 3), *heavy), -bound, bound).astype(held_as)


def setup_inputs(seed: int = 0, part: int = 0) -> dict:
    key_list = jax.random.split(jax.random.key(seed), 12)
    own_keys = jax.random.split(jax.random.fold_in(key_list[11], part), 12)
    return {
        "late_rows": bell_draw(own_keys[0], (TOKENS, D), 1.0, 6.0, ((0, 8),)),
        "early_rows": bell_draw_with(own_keys[1], (TOKENS, D), 1.0, 6.0, ((0, 8),), (0, 1, 8, 2.0)),
        "hidden_cot": bell_draw_with(own_keys[2], (TOKENS, FF), 1.0, 6.0, ((0, 8), (1, 2)), (0, 1, 8, 2.0)),
        "gate_weight": bell_draw(key_list[3], (D, FF), D ** -0.5, 0.125, ((0, 8), (1, 2))),
        "up_weight": bell_draw(key_list[4], (D, FF), D ** -0.5, 0.125, ((0, 8), (1, 2))),
        "gate_taps": bell_draw(key_list[5], (TAPS, FF), TAPS ** -0.5, 3.5, ((1, 2),)),
        "up_taps": bell_draw(key_list[6], (TAPS, FF), TAPS ** -0.5, 3.5, ((1, 2),)),
        "gate_grad_sum": bell_draw(own_keys[7], (D, FF), 1.0, 6.0, ((0, 8), (1, 2)), jnp.float32),
        "up_grad_sum": bell_draw(own_keys[8], (D, FF), 1.0, 6.0, ((0, 8), (1, 2)), jnp.float32),
        "gate_taps_sum": bell_draw(own_keys[9], (TAPS, FF), 1.0, 6.0, ((1, 2),), jnp.float32),
        "up_taps_sum": bell_draw(own_keys[10], (TAPS, FF), 1.0, 6.0, ((1, 2),), jnp.float32),
    }


def causal_mix(values, filter_taps):
    length = values.shape[-2]
    widths = [(0, 0)] * values.ndim
    widths[-2] = (2, 0)
    padded = jnp.pad(values, widths)
    return filter_taps[0] * padded[..., 0:length, :] + filter_taps[1] * padded[..., 1:length + 1, :] + filter_taps[2] * padded[..., 2:length + 2, :]

def mix_back(grads, filter_taps):
    length = grads.shape[-2]
    widths = [(0, 0)] * grads.ndim
    widths[-2] = (0, 2)
    padded = jnp.pad(grads, widths)
    return filter_taps[2] * padded[..., 0:length, :] + filter_taps[1] * padded[..., 1:length + 1, :] + filter_taps[0] * padded[..., 2:length + 2, :]

def tap_products(grads, values):
    length = values.shape[-2]
    widths = [(0, 0)] * values.ndim
    widths[-2] = (2, 0)
    padded = jnp.pad(values, widths)
    axes = tuple(range(values.ndim - 1))
    return jnp.stack([lax.optimization_barrier(jnp.sum(grads * padded[..., offset:offset + length, :], axis=axes)) for offset in range(3)])

def stored(product):
    return lax.optimization_barrier(product.astype(jnp.bfloat16)).astype(jnp.float32)

def reference(late_rows, early_rows, hidden_cot, gate_weight, up_weight, gate_taps, up_taps, gate_grad_sum, up_grad_sum, gate_taps_sum, up_taps_sum):
    rows_scale = TOKENS ** (-0.5)
    gate_filter = gate_taps.astype(jnp.float32)
    up_filter = up_taps.astype(jnp.float32)

    def project(source):
        gate_pre = stored(jnp.dot(source, gate_weight, preferred_element_type=jnp.float32))
        up_pre = stored(jnp.dot(source, up_weight, preferred_element_type=jnp.float32))
        return (gate_pre.reshape(N_FS, TOK_DEV, FF), up_pre.reshape(N_FS, TOK_DEV, FF))
    late_gate, late_up = project(late_rows)
    late_hidden = (jax.nn.gelu(causal_mix(late_gate, gate_filter), approximate=True) * causal_mix(late_up, up_filter)).astype(jnp.bfloat16).reshape(TOKENS, FF)
    early_gate, early_up = project(early_rows)
    gate_mix = causal_mix(early_gate, gate_filter)
    up_mix = causal_mix(early_up, up_filter)
    cotangent = hidden_cot.astype(jnp.float32).reshape(N_FS, TOK_DEV, FF)
    activated, gelu_back = jax.vjp(lambda mixed_value: jax.nn.gelu(mixed_value, approximate=True), gate_mix)
    d_gate_mix = gelu_back(cotangent * up_mix)[0]
    d_up_mix = cotangent * activated
    d_gate_pre = mix_back(d_gate_mix, gate_filter).astype(jnp.bfloat16)
    d_up_pre = mix_back(d_up_mix, up_filter).astype(jnp.bfloat16)
    gate_taps_next = gate_taps_sum + rows_scale * tap_products(d_gate_mix, early_gate)
    up_taps_next = up_taps_sum + rows_scale * tap_products(d_up_mix, early_up)
    flat_gate = d_gate_pre.reshape(TOKENS, FF)
    flat_up = d_up_pre.reshape(TOKENS, FF)
    early_grad = (jnp.dot(flat_gate, gate_weight.T, preferred_element_type=jnp.float32) + jnp.dot(flat_up, up_weight.T, preferred_element_type=jnp.float32)).astype(jnp.bfloat16)
    both_grads = jnp.concatenate([d_gate_pre, d_up_pre], axis=-1)
    blocks = early_rows.reshape(N_FS, TOK_DEV, D)

    def add_device(total, pair):
        block_rows, block_grads = pair
        term = (jnp.dot(block_rows.T, block_grads, preferred_element_type=jnp.float32) * rows_scale).astype(jnp.bfloat16)
        term = lax.optimization_barrier(term)
        return (total + term.astype(jnp.float32), None)
    summed = lax.scan(add_device, jnp.zeros((D, 2 * FF), jnp.float32), (blocks, both_grads))[0]
    return (late_hidden, early_grad, gate_grad_sum + summed[:, :FF], up_grad_sum + summed[:, FF:], gate_taps_next, up_taps_next)
```

```python
import jax
import jax.numpy as jnp
from jax import lax
from jax.sharding import PartitionSpec as P

contract_last = (((1,), (1,)), ((), ()))
contract_first = (((0,), (0,)), ((), ()))


def causal_mix(values, filter_taps):
    length = values.shape[-2]
    widths = [(0, 0)] * values.ndim
    widths[-2] = (2, 0)
    padded = jnp.pad(values, widths)
    return (
        filter_taps[0] * padded[..., 0:length, :]
        + filter_taps[1] * padded[..., 1 : length + 1, :]
        + filter_taps[2] * padded[..., 2 : length + 2, :]
    )


def mix_back(grads, filter_taps):
    length = grads.shape[-2]
    widths = [(0, 0)] * grads.ndim
    widths[-2] = (0, 2)
    padded = jnp.pad(grads, widths)
    return (
        filter_taps[2] * padded[..., 0:length, :]
        + filter_taps[1] * padded[..., 1 : length + 1, :]
        + filter_taps[0] * padded[..., 2 : length + 2, :]
    )


def tap_products(grads, values):
    length = values.shape[-2]
    widths = [(0, 0)] * values.ndim
    widths[-2] = (2, 0)
    padded = jnp.pad(values, widths)
    axes = tuple(range(values.ndim - 1))
    return jnp.stack(
        [
            jnp.sum(grads * padded[..., offset : offset + length, :], axis=axes)
            for offset in range(3)
        ]
    )


def stored(product):
    return lax.optimization_barrier(product.astype(jnp.bfloat16)).astype(jnp.float32)


def per_device(
    late_rows,
    early_rows,
    hidden_cot,
    gate_weight,
    up_weight,
    gate_taps,
    up_taps,
    gate_grad_sum,
    up_grad_sum,
    gate_taps_sum,
    up_taps_sum,
):
    row_count = late_rows.shape[0]
    width_local = gate_weight.shape[1]
    rows_scale = (row_count * lax.axis_size("fs")) ** (-0.5)
    gate_filter = gate_taps.astype(jnp.float32)
    up_filter = up_taps.astype(jnp.float32)
    joined_weight = jnp.concatenate([gate_weight, up_weight], axis=1)
    both_rows = jnp.concatenate([late_rows, early_rows], axis=0)
    whole_joined = lax.all_gather(joined_weight, "fs", axis=0, tiled=True)
    projected = jnp.dot(both_rows, whole_joined, preferred_element_type=jnp.float32)
    projected = stored(projected)
    late_gate = projected[:row_count, :width_local]
    late_up = projected[:row_count, width_local:]
    early_gate = projected[row_count:, :width_local]
    early_up = projected[row_count:, width_local:]
    late_hidden = (
        jax.nn.gelu(causal_mix(late_gate, gate_filter), approximate=True)
        * causal_mix(late_up, up_filter)
    ).astype(jnp.bfloat16)
    gate_mix = causal_mix(early_gate, gate_filter)
    up_mix = causal_mix(early_up, up_filter)
    cotangent = hidden_cot.astype(jnp.float32)
    activated, gelu_back = jax.vjp(
        lambda mixed_value: jax.nn.gelu(mixed_value, approximate=True), gate_mix
    )
    d_gate_mix = gelu_back(cotangent * up_mix)[0]
    d_up_mix = cotangent * activated
    d_gate_pre = mix_back(d_gate_mix, gate_filter).astype(jnp.bfloat16)
    d_up_pre = mix_back(d_up_mix, up_filter).astype(jnp.bfloat16)
    both_grads = jnp.concatenate([d_gate_pre, d_up_pre], axis=1)
    early_grad = lax.psum(
        lax.dot_general(
            both_grads, whole_joined, contract_last, preferred_element_type=jnp.float32
        ).astype(jnp.bfloat16),
        "tp",
    )
    summed = lax.psum_scatter(
        (
            lax.dot_general(
                early_rows, both_grads, contract_first, preferred_element_type=jnp.float32
            )
            * rows_scale
        ).astype(jnp.bfloat16),
        "fs",
        scatter_dimension=0,
        tiled=True,
    ).astype(jnp.float32)
    gate_tap_sums, up_tap_sums = lax.psum(
        (
            rows_scale * tap_products(d_gate_mix, early_gate),
            rows_scale * tap_products(d_up_mix, early_up),
        ),
        "fs",
    )
    return (
        late_hidden,
        early_grad,
        gate_grad_sum + summed[:, :width_local],
        up_grad_sum + summed[:, width_local:],
        gate_taps_sum + gate_tap_sums,
        up_taps_sum + up_tap_sums,
    )


def by_tokens(
    late_rows,
    early_rows,
    hidden_cot,
    gate_weight,
    up_weight,
    gate_taps,
    up_taps,
    gate_grad_sum,
    up_grad_sum,
    gate_taps_sum,
    up_taps_sum,
):
    fs_size = lax.axis_size("fs")
    tp_size = lax.axis_size("tp")
    turns = fs_size // tp_size
    row_count, model = late_rows.shape
    width = gate_weight.shape[1]
    part = width // fs_size
    rows_scale = (row_count * fs_size) ** (-0.5)
    chip = lax.axis_index("fs")
    core = lax.axis_index("tp")
    same = (chip % tp_size) == core

    def at(index_fs, index_tp):
        return (index_fs % fs_size) * tp_size + index_tp % tp_size

    def moved(value, target):
        pairs = []
        for f in range(fs_size):
            for t in range(tp_size):
                pairs.append((at(f, t), at(*target(f, t))))
        return lax.ppermute(value, ("fs", "tp"), pairs)

    def swapped(value):
        return lax.ppermute(value, "tp", [(0, 1), (1, 0)])

    def cut(value, index):
        return lax.dynamic_slice_in_dim(value, index * part, part, value.ndim - 1)

    def joined(own):
        return jnp.concatenate([own, swapped(own)], axis=-1)

    def parts_of(value):
        return value.reshape(value.shape[0], fs_size, part).transpose(1, 0, 2)

    packed = jnp.stack([parts_of(gate_weight), parts_of(up_weight)], axis=1)
    group = lax.axis_index("rep")
    depth = packed.shape[2] // 2
    packed = lax.dynamic_slice_in_dim(packed, group * depth, depth, 2)
    packed = lax.all_to_all(packed, "fs", 0, 0, tiled=True)
    facing = lax.ppermute(packed, "rep", [(0, 1), (1, 0)])
    packed = jnp.where(
        group == 0,
        jnp.concatenate([packed, facing], axis=2),
        jnp.concatenate([facing, packed], axis=2),
    )
    packed = packed.transpose(1, 0, 2, 3).reshape(2, model, part)
    both_weight = joined(packed)
    gate_whole, up_whole = both_weight[0], both_weight[1]
    taps = jnp.concatenate([cut(gate_taps, chip), cut(up_taps, chip)], axis=0)
    other_taps = swapped(jnp.concatenate([gate_taps, up_taps], axis=0))
    taps = jnp.concatenate([taps, cut(other_taps, chip)], axis=1)
    gate_filter = taps[:3].astype(jnp.float32)
    up_filter = taps[3:].astype(jnp.float32)

    def project(rows, weight):
        return stored(jnp.dot(rows, weight, preferred_element_type=jnp.float32))

    line = chip // tp_size
    column = chip % tp_size
    half_count = row_count // tp_size

    def half_of(value, index):
        return lax.dynamic_slice_in_dim(value, index * half_count, half_count, 0)

    def stepped(value, way):
        pairs = [
            (at(f, t), at(f + way * tp_size, t))
            for f in range(fs_size)
            for t in range(tp_size)
            if 0 <= f + way * tp_size < fs_size
        ]
        return lax.ppermute(value, ("fs", "tp"), pairs)

    def ordered(first, second, index):
        return jnp.where(
            index == 0,
            jnp.concatenate([first, second], axis=0),
            jnp.concatenate([second, first], axis=0),
        )

    def gathered(rows):
        held = half_of(rows, core)
        rising, falling = [held], [held]
        for _ in range(turns - 1):
            rising.append(stepped(rising[-1], 1))
            falling.append(stepped(falling[-1], -1))
        whole = []
        for k in range(turns):
            slot = held if k == 0 else jnp.where(line >= k, rising[k], falling[turns - k])
            halves = [
                moved(slot, lambda f, t, j=j: (f // tp_size * tp_size + (t + j) % tp_size, f))
                for j in range(tp_size)
            ]
            whole.append(ordered(halves[0], halves[1], column))
        return whole

    early_in = gathered(early_rows)
    late_in = gathered(late_rows)

    cot_in = []
    for k in range(turns):
        halves = []
        for j in range(tp_size):
            goal = (((chip // tp_size + k) * tp_size) + (core - j) % tp_size) % fs_size
            halves.append(
                moved(
                    cut(hidden_cot, goal),
                    lambda f, t, k=k, j=j: (
                        (f // tp_size + k) * tp_size + (t - j) % tp_size,
                        f,
                    ),
                )
            )
        first = jnp.where(same, halves[0], halves[1])
        second = jnp.where(same, halves[1], halves[0])
        cot_in.append(jnp.concatenate([first, second], axis=1))

    late_back = []
    for k in range(turns):
        hidden = (
            jax.nn.gelu(
                causal_mix(project(late_in[k], gate_whole), gate_filter), approximate=True
            )
            * causal_mix(project(late_in[k], up_whole), up_filter)
        ).astype(jnp.bfloat16)
        own, other = hidden[:, :part], hidden[:, part:]
        for j in range(tp_size):
            piece = jnp.where(same, own, other) if j == 0 else jnp.where(same, other, own)
            late_back.append(
                moved(
                    piece,
                    lambda f, t, k=k, j=j: ((f // tp_size - k) * tp_size + t, f + j),
                )
            )
    late_stack = jnp.stack(late_back)
    pieces = []
    for g in range(fs_size):
        k = (g // tp_size - chip // tp_size) % turns
        j = (core - g) % tp_size
        pieces.append(
            lax.dynamic_index_in_dim(late_stack, k * tp_size + j, 0, keepdims=False)
        )
    late_hidden = jnp.concatenate(pieces, axis=1)

    early_sum = jnp.zeros((half_count, model), jnp.float32)
    d_gates, d_ups = [], []
    tap_sums = jnp.zeros((6, 2 * part), jnp.float32)
    for k in range(turns):
        early_gate = project(early_in[k], gate_whole)
        early_up = project(early_in[k], up_whole)
        gate_mix = causal_mix(early_gate, gate_filter)
        up_mix = causal_mix(early_up, up_filter)
        cotangent = cot_in[k].astype(jnp.float32)
        activated, gelu_back = jax.vjp(
            lambda mixed_value: jax.nn.gelu(mixed_value, approximate=True), gate_mix
        )
        d_gate_mix = gelu_back(cotangent * up_mix)[0]
        d_up_mix = cotangent * activated
        d_gate_pre = mix_back(d_gate_mix, gate_filter).astype(jnp.bfloat16)
        d_up_pre = mix_back(d_up_mix, up_filter).astype(jnp.bfloat16)
        d_gates.append(d_gate_pre)
        d_ups.append(d_up_pre)
        tap_sums = tap_sums + jnp.concatenate(
            [tap_products(d_gate_mix, early_gate), tap_products(d_up_mix, early_up)]
        )
        share = lax.dot_general(
            d_gate_pre, gate_whole, contract_last, preferred_element_type=jnp.float32
        ) + lax.dot_general(
            d_up_pre, up_whole, contract_last, preferred_element_type=jnp.float32
        )
        share = share.astype(jnp.bfloat16)
        pair_sum = sum(
            moved(
                half_of(share, (column + j) % tp_size),
                lambda f, t, j=j: (f // tp_size * tp_size + t, f + j),
            ).astype(jnp.float32)
            for j in range(tp_size)
        )
        if k:
            pair_sum = moved(
                pair_sum.astype(jnp.bfloat16), lambda f, t, k=k: (f - k * tp_size, t)
            ).astype(jnp.float32)
        early_sum = early_sum + pair_sum
    early_half = early_sum.astype(jnp.bfloat16)
    early_grad = ordered(early_half, swapped(early_half), core)

    rows_joined = jnp.concatenate(early_in, axis=0)

    def weight_terms(grads):
        product = rows_scale * lax.dot_general(
            rows_joined,
            jnp.concatenate(grads, axis=0),
            contract_first,
            preferred_element_type=jnp.float32,
        )
        return product[:, :part], product[:, part:].astype(jnp.bfloat16)

    gate_own, gate_other = weight_terms(d_gates)
    up_own, up_other = weight_terms(d_ups)
    arrived = swapped(jnp.stack([gate_other, up_other]))
    summed = (jnp.stack([gate_own, up_own]) + arrived.astype(jnp.float32)).astype(
        jnp.bfloat16
    )
    summed = summed.reshape(2, fs_size, model // fs_size, part).transpose(1, 0, 2, 3)
    summed = lax.all_to_all(summed, "fs", 0, 0, tiled=True)
    summed = summed.transpose(1, 2, 0, 3).reshape(2, model // fs_size, width)
    summed = summed.astype(jnp.float32)

    tap_sums = rows_scale * (tap_sums[:, :part] + swapped(tap_sums[:, part:]))
    tap_all = jnp.broadcast_to(tap_sums, (fs_size,) + tap_sums.shape)
    tap_all = lax.all_to_all(tap_all, "fs", 0, 0, tiled=True)
    tap_all = tap_all.transpose(1, 0, 2).reshape(6, width)
    return (
        late_hidden,
        early_grad,
        gate_grad_sum + summed[0],
        up_grad_sum + summed[1],
        gate_taps_sum + tap_all[:3],
        up_taps_sum + tap_all[3:],
    )


def solution(mesh):
    in_specs = (
        P(("rep", "fs"), None),
        P(("rep", "fs"), None),
        P(("rep", "fs"), "tp"),
        P("fs", "tp"),
        P("fs", "tp"),
        P(None, "tp"),
        P(None, "tp"),
        P(("rep", "fs"), "tp"),
        P(("rep", "fs"), "tp"),
        P("rep", "tp"),
        P("rep", "tp"),
    )
    out_specs = (
        P(("rep", "fs"), "tp"),
        P(("rep", "fs"), None),
        P(("rep", "fs"), "tp"),
        P(("rep", "fs"), "tp"),
        P("rep", "tp"),
        P("rep", "tp"),
    )
    fs_size, tp_size = mesh.shape["fs"], mesh.shape["tp"]

    def run(*args):
        tokens = args[0].shape[0] // mesh.shape["rep"]
        width = args[3].shape[1] // tp_size
        few = 3 * tokens < 4 * tp_size * width and width % fs_size == 0
        fits = tp_size == 2 and mesh.shape["rep"] == 2 and fs_size % 2 == 0 and few
        return jax.shard_map(
            by_tokens if fits else per_device,
            mesh=mesh,
            in_specs=in_specs,
            out_specs=out_specs,
            check_vma=False,
        )(*args)

    return run
```
